32 devices in a mesh: grp: 2 (over y), fs: 4 (over z), tp: 4 (over x, core).
Axes of the slice: x: 2, y: 2, z: 4, core: 2. Of those that a mesh axis runs over, the one named last changes fastest.
Arguments:
- tokens: bfloat16 [8, 1024, 2048], P(('grp', 'fs'), None, 'tp'), parts along dimension 0, may hold values from -6 to 6
- mix_gain: float32 [2048], replicated, may hold values from 0.1 to 1.9
- in_matrix: float32 [2048, 1024], P('fs', 'tp'), may hold values from -0.125 to 0.125
- in_scale: float32 [1, 1024], P(None, 'tp'), may hold values from 0.5 to 2
- pool_mix: bfloat16 [8, 128, 128], P('tp'), may hold values from -0.5 to 0.5
- pool_scale: float32 [1, 1024], P(None, 'tp'), may hold values from 0.1 to 1.9
- out_matrix: float32 [1024, 2048], P('tp', 'fs'), may hold values from -0.25 to 0.25
- out_scale: float32 [1, 2048], P(None, 'fs'), may hold values from 0.5 to 2
- ffn_gain: float32 [2048], replicated, may hold values from 0.1 to 1.9
- gate_matrix: float32 [2048, 5632], P('fs', 'tp'), may hold values from -0.125 to 0.125
- gate_scale: float32 [1, 5632], P(None, 'tp'), may hold values from 0.5 to 2
- up_matrix: float32 [2048, 5632], P('fs', 'tp'), may hold values from -0.125 to 0.125
- up_scale: float32 [1, 5632], P(None, 'tp'), may hold values from 0.5 to 2
- gate_taps: float32 [3, 5632], P(None, 'tp'), may hold values from -4 to 4
- up_taps: float32 [3, 5632], P(None, 'tp'), may hold values from -4 to 4
- down_matrix: float32 [5632, 2048], P('tp', 'fs'), may hold values from -0.109375 to 0.109375
- down_scale: float32 [1, 2048], P(None, 'fs'), may hold values from 0.5 to 2
Outputs:
- layer_out: bfloat16 [8, 1024, 2048], P(('grp', 'fs'), None, 'tp'), parts along dimension 0
The draws below stay inside these ranges and needn't reach their ends.
There are 2 independent parts, one for each index of `grp`. The reference program is written for one: setup_inputs(seed, part) draws one part's arguments, and reference() takes and returns one part's arrays. A program takes and returns all parts, laid end to end along the dimension named above; an argument that names none is the same for every part. Nothing has to cross between parts.
All inputs are finite; a program needn't handle non-finite values.
Results may differ from the reference program's by a relative error of at most 0.025.
Values may be sent and summed in bfloat16 or wider, within the bound.
No kernel may reach another device: no remote copies, remote signals or barrier semaphores. Data moves between devices by JAX's collectives and lax.ppermute only.
A program may use at most 128 MiB of HBM per device.

```python
import math
import jax
import jax.numpy as jnp
from jax import lax

D = 2048
BLOCKS = 8
BLOCK_CH = 128
FF = 5632
LEN = 1024
PW = 1024
SEQS = 4
COL_GROUPS = 4


def raised(array, stream_key, source, target, shards_of, factor):
    def block_of(dim):
        return (jnp.arange(array.shape[dim]) // (array.shape[dim] // shards_of)).reshape((-1,) + (1,) * (array.ndim - 1 - dim))

    near = jax.random.permutation(stream_key, shards_of)[block_of(target)]
    far = (block_of(target) + shards_of // 2) % shards_of
    return jnp.where((block_of(source) == near) | (block_of(source) == far), factor * array, array)


def levels(stream_key, shape, pieces, least, top_value):
    level, own = 1.0, jax.random.fold_in(stream_key, 6)
    for dim, shards_of in pieces:
        steps = jnp.exp(jax.random.uniform(jax.random.fold_in(own, dim), (shards_of,), jnp.float32, least / len(pieces), top_value / len(pieces)))
        level = level * jnp.repeat(steps, shape[dim] // shards_of).reshape([-1 if axis == dim else 1 for axis in range(len(shape))])
    return level


def bell_draw(own_key, shape, deviation, reach, pieces=(), kind=jnp.bfloat16):
    drawn = deviation * jax.random.normal(own_key, shape, jnp.float32)
    if pieces:
        drawn = drawn * levels(own_key, shape, pieces, -0.22, 0.18)
    return jnp.clip(drawn, -reach, reach).astype(kind)


def gaussian_with(rng, shape, width, reach, cuts, heavy, held_as=jnp.bfloat16):
    drawn = width * jax.random.normal(rng, shape, jnp.float32)
    if cuts:
        drawn = drawn * levels(rng, shape, cuts, -0.22, 0.18)
    return jnp.clip(raised(drawn, jax.random.fold_in(rng, 3), *heavy), -reach, reach).astype(held_as)


def setup_inputs(seed: int = 0, part: int = 0) -> dict:
    streams_of = jax.random.split(jax.random.key(seed), 18)
    part_keys = jax.random.split(jax.random.fold_in(streams_of[17], part), 18)
    tokens = bell_draw(part_keys[0], (SEQS, LEN, D), 1.0, 6.0, ((0, 4), (2, 4)))
    mix_gain = jnp.clip(1.0 + 0.18 * jax.random.normal(streams_of[1], (D,), jnp.float32), 0.1, 1.9)
    in_matrix = bell_draw(streams_of[2], (D, PW), D ** -0.5, 0.125, ((0, 4), (1, 4)), jnp.float32)
    in_scale = jnp.clip(jnp.exp(math.log(2.0) - 1.3862944 * jax.random.uniform(streams_of[3], (1, PW), jnp.float32) ** levels(streams_of[3], (1, PW), ((1, 4),), -0.2, 0.2)), 0.5, 2.0)
    pool_mix = bell_draw(streams_of[4], (BLOCKS, BLOCK_CH, BLOCK_CH), BLOCK_CH ** -0.5, 0.5, ((0, 4),))
    pool_scale = jnp.clip(1.0 + 0.18 * jax.random.normal(streams_of[5], (1, PW), jnp.float32), 0.1, 1.9)
    out_matrix = gaussian_with(streams_of[6], (PW, D), PW ** -0.5, 0.25, ((0, 4), (1, 4)), (0, 1, 4, 2.0), jnp.float32)
    out_scale = jnp.clip(jnp.exp(math.log(2.0) - 1.3862944 * jax.random.uniform(streams_of[7], (1, D), jnp.float32) ** levels(streams_of[7], (1, D), ((1, 4),), -0.2, 0.2)), 0.5, 2.0)
    ffn_gain = jnp.clip(1.0 + 0.18 * jax.random.normal(streams_of[8], (D,), jnp.float32), 0.1, 1.9)
    gate_matrix = bell_draw(streams_of[9], (D, FF), D ** -0.5, 0.125, ((0, 4), (1, 4)), jnp.float32)
    gate_scale = jnp.clip(jnp.exp(math.log(2.0) - 1.3862944 * jax.random.uniform(streams_of[10], (1, FF), jnp.float32) ** levels(streams_of[10], (1, FF), ((1, 4),), -0.2, 0.2)), 0.5, 2.0)
    up_matrix = bell_draw(streams_of[11], (D, FF), D ** -0.5, 0.125, ((0, 4), (1, 4)), jnp.float32)
    up_scale = jnp.clip(jnp.exp(math.log(2.0) - 1.3862944 * jax.random.uniform(streams_of[12], (1, FF), jnp.float32) ** levels(streams_of[12], (1, FF), ((1, 4),), -0.2, 0.2)), 0.5, 2.0)
    gate_taps = bell_draw(streams_of[13], (3, FF), 0.58, 4.0, ((1, 4),), jnp.float32)
    up_taps = bell_draw(streams_of[14], (3, FF), 0.58, 4.0, ((1, 4),), jnp.float32)
    down_matrix = gaussian_with(streams_of[15], (FF, D), FF ** -0.5, 0.109375, ((0, 4), (1, 4)), (0, 1, 4, 2.0), jnp.float32)
    down_scale = jnp.clip(jnp.exp(math.log(2.0) - 1.3862944 * jax.random.uniform(streams_of[16], (1, D), jnp.float32) ** levels(streams_of[16], (1, D), ((1, 4),), -0.2, 0.2)), 0.5, 2.0)
    return {"tokens": tokens, "mix_gain": mix_gain, "in_matrix": in_matrix, "in_scale": in_scale, "pool_mix": pool_mix, "pool_scale": pool_scale, "out_matrix": out_matrix, "out_scale": out_scale, "ffn_gain": ffn_gain, "gate_matrix": gate_matrix, "gate_scale": gate_scale, "up_matrix": up_matrix, "up_scale": up_scale, "gate_taps": gate_taps, "up_taps": up_taps, "down_matrix": down_matrix, "down_scale": down_scale}


eps = 1e-06
widest_span = 16

def norm_rows(tok_rows, norm_gain):
    values = tok_rows.astype(jnp.float32)
    scaled = values * lax.rsqrt(lax.optimization_barrier(jnp.mean(values * values, axis=-1, keepdims=True)) + eps)
    return (scaled * norm_gain.astype(jnp.float32)).astype(jnp.bfloat16)

def span_widths(block_ids):
    return jnp.left_shift(jnp.ones_like(block_ids), (1 + 4 * block_ids // BLOCKS).astype(jnp.int32))

def trailing_gap(projected, windows):
    values = projected.astype(jnp.float32)
    length = values.shape[0]
    running = values
    for offset in range(1, widest_span):
        shifted = jnp.pad(values[:length - offset], ((offset, 0), (0, 0)))
        running = running + jnp.where(windows[None, :] > offset, shifted, jnp.zeros_like(shifted))
    positions = jnp.arange(length, dtype=jnp.int32)[:, None]
    counts = jnp.minimum(positions + 1, windows[None, :]).astype(jnp.float32)
    return (running / counts - values).astype(jnp.bfloat16)

def causal_taps(linear, tap_table):
    values = linear.astype(jnp.float32)
    length = values.shape[0]
    back_one = jnp.pad(values[:length - 1], ((1, 0), (0, 0)))
    back_two = jnp.pad(values[:length - 2], ((2, 0), (0, 0)))
    return tap_table[2] * values + tap_table[1] * back_one + tap_table[0] * back_two

def grouped_product(operand, matrix, scales):
    narrow = operand.shape[1] // COL_GROUPS
    cast_matrix = matrix.astype(jnp.bfloat16)
    running = jnp.zeros((operand.shape[0], matrix.shape[1]), jnp.float32)
    for member in range(COL_GROUPS):
        partial_value = jnp.dot(operand[:, member * narrow:(member + 1) * narrow], cast_matrix[member * narrow:(member + 1) * narrow], preferred_element_type=jnp.float32) * scales
        rounded = lax.optimization_barrier(partial_value.astype(jnp.bfloat16))
        running = running + rounded.astype(jnp.float32)
    return running

def reference(tokens, mix_gain, in_matrix, in_scale, pool_mix, pool_scale, out_matrix, out_scale, ffn_gain, gate_matrix, gate_scale, up_matrix, up_scale, gate_taps, up_taps, down_matrix, down_scale):
    windows = jnp.repeat(span_widths(jnp.arange(BLOCKS, dtype=jnp.int32)), BLOCK_CH)
    in_cast = in_matrix.astype(jnp.bfloat16)
    gate_cast = gate_matrix.astype(jnp.bfloat16)
    up_cast = up_matrix.astype(jnp.bfloat16)

    def single(sequence):
        normed = norm_rows(sequence, mix_gain)
        projected = (jnp.dot(normed, in_cast, preferred_element_type=jnp.float32) * in_scale).astype(jnp.bfloat16)
        spread = trailing_gap(projected, windows)
        blocks = spread.reshape(-1, BLOCKS, BLOCK_CH).astype(jnp.float32)
        block_mixed = jnp.einsum('lbc,bce->lbe', blocks, pool_mix.astype(jnp.float32)).reshape(-1, PW)
        pooled = (block_mixed * pool_scale).astype(jnp.bfloat16)
        mixing = grouped_product(pooled, out_matrix, out_scale)
        residual = (sequence.astype(jnp.float32) + mixing).astype(jnp.bfloat16)
        normed_ffn = norm_rows(residual, ffn_gain)
        gate_lin = (jnp.dot(normed_ffn, gate_cast, preferred_element_type=jnp.float32) * gate_scale).astype(jnp.bfloat16)
        up_lin = (jnp.dot(normed_ffn, up_cast, preferred_element_type=jnp.float32) * up_scale).astype(jnp.bfloat16)
        hidden = (jax.nn.silu(causal_taps(gate_lin, gate_taps)) * causal_taps(up_lin, up_taps)).astype(jnp.bfloat16)
        feed_out = grouped_product(hidden, down_matrix, down_scale)
        return (residual.astype(jnp.float32) + feed_out).astype(jnp.bfloat16)
    return lax.map(single, tokens)
```

```python
import jax
import jax.numpy as jnp
from jax import lax
from jax.sharding import PartitionSpec as P

BLOCKS = 8


eps = 1e-06
widest_span = 16


def norm_rows(tok_rows, norm_gain):
    values = tok_rows.astype(jnp.float32)
    scaled = values * lax.rsqrt(jnp.mean(values * values, axis=-1, keepdims=True) + eps)
    return (scaled * norm_gain).astype(jnp.bfloat16)


def span_widths(block_ids):
    return jnp.left_shift(jnp.ones_like(block_ids), 1 + 4 * block_ids // BLOCKS)


def trailing_gap(projected, windows):
    values = projected.astype(jnp.float32)
    length = values.shape[0]
    running = values
    for offset in range(1, widest_span):
        shifted = jnp.pad(values[: length - offset], ((offset, 0), (0, 0)))
        running = running + jnp.where(windows[None, :] > offset, shifted, jnp.zeros_like(shifted))
    positions = jnp.arange(length, dtype=jnp.int32)[:, None]
    counts = jnp.minimum(positions + 1, windows[None, :]).astype(jnp.float32)
    return (running / counts - values).astype(jnp.bfloat16)


def causal_taps(linear, tap_table):
    values = linear.astype(jnp.float32)
    length = values.shape[0]
    back_one = jnp.pad(values[: length - 1], ((1, 0), (0, 0)))
    back_two = jnp.pad(values[: length - 2], ((2, 0), (0, 0)))
    return tap_table[2] * values + tap_table[1] * back_one + tap_table[0] * back_two


def fold_rows(operand, portion):
    return jnp.dot(operand, portion, preferred_element_type=jnp.float32)


def tp_swap(value):
    size = lax.axis_size("tp")
    return lax.ppermute(value, "tp", [(i, i ^ 1) for i in range(size)])


def tp_step(value, step):
    size = lax.axis_size("tp")
    chips = size // 2
    pairs = [(i, ((i // 2 + step) % chips) * 2 + i % 2) for i in range(size)]
    return lax.ppermute(value, "tp", pairs)


def tp_pieces(value):
    chips = lax.axis_size("tp") // 2
    near = [value] + [tp_step(value, step) for step in range(1, chips)]
    pieces = []
    for piece in near:
        pieces += [piece, tp_swap(piece)]
    return pieces


def tp_sources():
    chips = lax.axis_size("tp") // 2
    index = lax.axis_index("tp")
    ids = []
    for step in range(chips):
        chip = (index // 2 + chips - step) % chips
        ids += [chip * 2 + index % 2, chip * 2 + 1 - index % 2]
    return ids


def pick_blocks(array, ids, axis=0):
    width = array.shape[axis] // len(ids)
    return jnp.concatenate(
        [lax.dynamic_slice_in_dim(array, i * width, width, axis) for i in ids], axis
    )


def part_columns(array, which, parts):
    width = array.shape[1] // parts
    chosen = array[:, :width]
    for i in range(1, parts):
        chosen = jnp.where(which == i, array[:, i * width : (i + 1) * width], chosen)
    return chosen


def column_block(stacked, index, blocks):
    count, rows, width = stacked.shape
    if count % blocks == 0:
        n = count // blocks
        taken = lax.dynamic_slice_in_dim(stacked, index * n, n, 0)
        return jnp.moveaxis(taken, 0, 1).reshape(rows, n * width)
    whole = jnp.moveaxis(stacked, 0, 1).reshape(rows, count * width)
    own = count * width // blocks
    return lax.dynamic_slice_in_dim(whole, index * own, own, 1)


def shards(
    tokens,
    mix_gain,
    in_matrix,
    in_scale,
    pool_mix,
    pool_scale,
    out_matrix,
    out_scale,
    ffn_gain,
    gate_matrix,
    gate_scale,
    up_matrix,
    up_scale,
    gate_taps,
    up_taps,
    down_matrix,
    down_scale,
):
    length = tokens.shape[1]
    own_width = tokens.shape[2]
    bf16 = jnp.bfloat16
    tp_index = lax.axis_index("tp")
    tp_size = lax.axis_size("tp")
    group = lax.axis_index("grp")
    parts = lax.axis_size("grp")
    ids = tp_sources()
    local_rows = tokens.reshape(length, own_width)
    gathered = jnp.concatenate(tp_pieces(local_rows), axis=1)

    in_full = lax.all_gather(in_matrix.astype(bf16), "fs", axis=0, tiled=True)
    out_rows = lax.all_gather((out_matrix * out_scale).astype(bf16), "fs", axis=1, tiled=True)
    own_matrix = lax.all_to_all(out_rows, "tp", split_axis=1, concat_axis=0, tiled=True)

    def across_groups(held):
        size = parts
        return [held] + [
            lax.ppermute(held, "grp", [(i, (i - step) % size) for i in range(size)])
            for step in range(1, size)
        ]

    gate_part = part_columns(gate_matrix, group, parts).astype(bf16)
    up_part = part_columns(up_matrix, group, parts).astype(bf16)
    down_height = down_matrix.shape[0] // parts
    down_part = lax.dynamic_slice_in_dim(down_matrix, group * down_height, down_height, 0)
    down_part = (down_part * down_scale).astype(bf16)
    gate_parts = across_groups(lax.all_gather(gate_part, "fs", axis=0, tiled=True))
    up_parts = across_groups(lax.all_gather(up_part, "fs", axis=0, tiled=True))
    down_parts = across_groups(lax.all_gather(down_part, "fs", axis=0, tiled=False))

    normed = norm_rows(gathered, pick_blocks(mix_gain, ids))
    width_in = in_matrix.shape[1]
    projected = (fold_rows(normed, pick_blocks(in_full, ids)) * in_scale).astype(bf16)
    local_blocks = pool_mix.shape[0]
    block_width = pool_mix.shape[1]
    block_ids = tp_index * local_blocks + jnp.arange(local_blocks, dtype=jnp.int32)
    windows = jnp.repeat(span_widths(block_ids), block_width)
    spread = trailing_gap(projected, windows)
    block_mixed = jnp.einsum(
        "lbc,bce->lbe",
        spread.reshape(length, local_blocks, block_width),
        pool_mix,
        preferred_element_type=jnp.float32,
    ).reshape(length, width_in)
    pooled = (block_mixed * pool_scale).astype(bf16)
    pooled_all = jnp.concatenate(tp_pieces(pooled), axis=1)
    mixing = fold_rows(pooled_all, pick_blocks(own_matrix, ids))
    residual = (local_rows.astype(jnp.float32) + mixing).astype(bf16)

    gathered_ffn = jnp.concatenate(tp_pieces(residual), axis=1)
    normed_ffn = norm_rows(gathered_ffn, pick_blocks(ffn_gain, ids))
    hidden_parts = []
    for step in range(parts):
        which = (group + step) % parts
        gate_total = fold_rows(normed_ffn, pick_blocks(gate_parts[step], ids))
        up_total = fold_rows(normed_ffn, pick_blocks(up_parts[step], ids))
        gate_lin = (gate_total * part_columns(gate_scale, which, parts)).astype(bf16)
        up_lin = (up_total * part_columns(up_scale, which, parts)).astype(bf16)
        gate_conv = causal_taps(gate_lin, part_columns(gate_taps, which, parts))
        up_conv = causal_taps(up_lin, part_columns(up_taps, which, parts))
        hidden_parts.append((jax.nn.silu(gate_conv) * up_conv).astype(bf16))

    def down_product(index):
        total = None
        for hidden, stacked in zip(hidden_parts, down_parts):
            piece = fold_rows(hidden, column_block(stacked, index, tp_size))
            total = piece if total is None else total + piece
        return total

    chips = tp_size // 2
    chip, core = tp_index // 2, tp_index % 2
    feed_out = jnp.zeros((length, own_width), jnp.float32)
    for step in list(range(1, chips)) + [0]:
        target = (chip + step) % chips
        other = tp_swap(down_product(target * 2 + 1 - core).astype(bf16))
        summed = down_product(target * 2 + core) + other.astype(jnp.float32)
        if step:
            summed = tp_step(summed.astype(bf16), step).astype(jnp.float32)
        feed_out = feed_out + summed
    result = (residual.astype(jnp.float32) + feed_out).astype(bf16)
    return result.reshape(1, length, result.shape[1])


def solution(mesh):
    return jax.shard_map(
        shards,
        mesh=mesh,
        in_specs=(
            P(("grp", "fs"), None, "tp"),
            P(),
            P("fs", "tp"),
            P(None, "tp"),
            P("tp", None, None),
            P(None, "tp"),
            P("tp", "fs"),
            P(None, "fs"),
            P(),
            P("fs", "tp"),
            P(None, "tp"),
            P("fs", "tp"),
            P(None, "tp"),
            P(None, "tp"),
            P(None, "tp"),
            P("tp", "fs"),
            P(None, "fs"),
        ),
        out_specs=P(("grp", "fs"), None, "tp"),
        check_vma=False,
    )
```

```python
import jax
import jax.numpy as jnp
from jax import lax
from jax.sharding import PartitionSpec as P


BLOCKS = 8


eps = 1e-06
widest_span = 16


def norm_rows(tok_rows, norm_gain):
    values = tok_rows.astype(jnp.float32)
    scaled = values * lax.rsqrt(jnp.mean(values * values, axis=-1, keepdims=True) + eps)
    return (scaled * norm_gain).astype(jnp.bfloat16)


def span_widths(block_ids):
    return jnp.left_shift(jnp.ones_like(block_ids), 1 + 4 * block_ids // BLOCKS)


def trailing_gap(projected, windows):
    values = projected.astype(jnp.float32)
    length = values.shape[0]
    running = values
    for offset in range(1, widest_span):
        shifted = jnp.pad(values[: length - offset], ((offset, 0), (0, 0)))
        running = running + jnp.where(windows[None, :] > offset, shifted, jnp.zeros_like(shifted))
    positions = jnp.arange(length, dtype=jnp.int32)[:, None]
    counts = jnp.minimum(positions + 1, windows[None, :]).astype(jnp.float32)
    return (running / counts - values).astype(jnp.bfloat16)


def causal_taps(linear, tap_table):
    values = linear.astype(jnp.float32)
    length = values.shape[0]
    back_one = jnp.pad(values[: length - 1], ((1, 0), (0, 0)))
    back_two = jnp.pad(values[: length - 2], ((2, 0), (0, 0)))
    return tap_table[2] * values + tap_table[1] * back_one + tap_table[0] * back_two


def fold_rows(operand, portion):
    return jnp.dot(operand, portion, preferred_element_type=jnp.float32)


def tp_swap(value):
    size = lax.axis_size("tp")
    return lax.ppermute(value, "tp", [(i, i ^ 1) for i in range(size)])


def tp_step(value, step):
    size = lax.axis_size("tp")
    chips = size // 2
    pairs = [(i, ((i // 2 + step) % chips) * 2 + i % 2) for i in range(size)]
    return lax.ppermute(value, "tp", pairs)


def tp_pieces(value):
    chips = lax.axis_size("tp") // 2
    near = [value] + [tp_step(value, step) for step in range(1, chips)]
    pieces = []
    for piece in near:
        pieces += [piece, tp_swap(piece)]
    return pieces


def tp_sources():
    chips = lax.axis_size("tp") // 2
    index = lax.axis_index("tp")
    ids = []
    for step in range(chips):
        chip = (index // 2 + chips - step) % chips
        ids += [chip * 2 + index % 2, chip * 2 + 1 - index % 2]
    return ids


def pick_blocks(array, ids, axis=0):
    width = array.shape[axis] // len(ids)
    return jnp.concatenate(
        [lax.dynamic_slice_in_dim(array, i * width, width, axis) for i in ids], axis
    )


def part_slice(array, which, parts, axis):
    width = array.shape[axis] // parts
    return lax.dynamic_slice_in_dim(array, which * width, width, axis)


def part_columns(array, which, parts):
    width = array.shape[1] // parts
    chosen = array[:, :width]
    for i in range(1, parts):
        chosen = jnp.where(which == i, array[:, i * width : (i + 1) * width], chosen)
    return chosen


def fs_stack(value):
    size = lax.axis_size("fs")
    index = lax.axis_index("fs")
    if size > 4:
        return lax.all_gather(value, "fs", axis=0, tiled=False), lambda j: j
    pieces = [value]
    for step in range(1, size):
        pairs = [(i, (i + step) % size) for i in range(size)]
        pieces.append(lax.ppermute(value, "fs", pairs))
    return jnp.stack(pieces), lambda j: (index - j + size) % size


def others_of(stacked):
    size = lax.axis_size("fs")
    index = lax.axis_index("fs")
    return jnp.concatenate(
        [lax.dynamic_slice_in_dim(stacked, (index + d) % size, 1, 0) for d in range(1, size)], 0
    )


def across_groups(sent, own_parts):
    parts = lax.axis_size("grp")
    found = []
    for step in range(1, parts):
        got = lax.ppermute(sent, "grp", [(i, (i - step) % parts) for i in range(parts)])
        found.append(jnp.concatenate([own_parts[step][None], got], 0))
    return found


def after(value, *earlier):
    return lax.optimization_barrier((value, *earlier))[0]


def rel_place(j):
    size = lax.axis_size("fs")
    return (j - lax.axis_index("fs") + size) % size


def row_blocks(stacked, ids, place):
    count = stacked.shape[0] // len(ids)
    return [
        lax.dynamic_slice_in_dim(stacked, place(i * count + j), 1, 0)[0]
        for i in ids
        for j in range(count)
    ]


def column_block(stacked, block, place):
    count = stacked.shape[0] // lax.axis_size("tp")
    return jnp.concatenate(row_blocks_of(stacked, block, count, place), axis=1)


def row_blocks_of(stacked, block, count, place):
    return [
        lax.dynamic_slice_in_dim(stacked, place(block * count + j), 1, 0)[0] for j in range(count)
    ]


def shards(
    tokens,
    mix_gain,
    in_matrix,
    in_scale,
    pool_mix,
    pool_scale,
    out_matrix,
    out_scale,
    ffn_gain,
    gate_matrix,
    gate_scale,
    up_matrix,
    up_scale,
    gate_taps,
    up_taps,
    down_matrix,
    down_scale,
):
    return layer(
        tokens,
        mix_gain,
        in_matrix,
        in_scale,
        pool_mix,
        pool_scale,
        out_matrix * out_scale,
        ffn_gain,
        gate_matrix,
        gate_scale,
        up_matrix,
        up_scale,
        gate_taps,
        up_taps,
        down_matrix * down_scale,
    )


def layer(
    tokens,
    mix_gain,
    in_matrix,
    in_scale,
    pool_mix,
    pool_scale,
    out_scaled,
    ffn_gain,
    gate_matrix,
    gate_scale,
    up_matrix,
    up_scale,
    gate_taps,
    up_taps,
    down_scaled,
):
    length = tokens.shape[1]
    own_width = tokens.shape[2]
    bf16 = jnp.bfloat16
    tp_index = lax.axis_index("tp")
    tp_size = lax.axis_size("tp")
    fs_size = lax.axis_size("fs")
    group = lax.axis_index("grp")
    parts = lax.axis_size("grp")
    ids = tp_sources()
    local_rows = tokens.reshape(length, own_width)
    gathered = jnp.concatenate(tp_pieces(local_rows), axis=1)
    in_stack, in_place = fs_stack(in_matrix.astype(bf16))
    out_stack, out_place = fs_stack(out_scaled.astype(bf16))

    whichs = [(group + step) % parts for step in range(parts)]
    gate_own = [part_slice(gate_matrix, which, parts, 0).astype(bf16) for which in whichs]
    up_own = [part_slice(up_matrix, which, parts, 0).astype(bf16) for which in whichs]
    half_width = down_scaled.shape[1] // parts
    chunks = 2 if half_width % 256 == 0 else 1
    chunk_width = half_width // chunks
    down_own = []
    for chunk in range(chunks):
        held = []
        for which in whichs:
            half = part_columns(down_scaled, which, parts).astype(bf16)
            held.append(half[:, chunk * chunk_width : (chunk + 1) * chunk_width])
        down_own.append(held)

    def gather(value):
        return lax.all_gather(value, "fs", axis=0, tiled=False)

    gate_mine = gather(gate_own[0])
    up_mine = gather(up_own[0])
    down_mine = [gather(down_own[c][0]) for c in range(chunks)]

    normed = norm_rows(gathered, pick_blocks(mix_gain, ids))
    width_in = in_matrix.shape[1]
    in_rows = jnp.concatenate(row_blocks(in_stack, ids, in_place), axis=0)
    projected = (fold_rows(normed, in_rows) * in_scale).astype(bf16)
    local_blocks = pool_mix.shape[0]
    block_width = pool_mix.shape[1]
    block_ids = tp_index * local_blocks + jnp.arange(local_blocks, dtype=jnp.int32)
    windows = jnp.repeat(span_widths(block_ids), block_width)
    spread = trailing_gap(projected, windows)
    block_mixed = jnp.einsum(
        "lbc,bce->lbe",
        spread.reshape(length, local_blocks, block_width),
        pool_mix,
        preferred_element_type=jnp.float32,
    ).reshape(length, width_in)
    pooled = (block_mixed * pool_scale).astype(bf16)
    out_blocks = jnp.stack([column_block(out_stack, i, out_place) for i in range(tp_size)])
    own_matrix = lax.all_to_all(out_blocks, "tp", split_axis=0, concat_axis=0, tiled=True)
    pooled_all = jnp.concatenate(tp_pieces(pooled), axis=1)
    out_pieces = [lax.dynamic_slice_in_dim(own_matrix, i, 1, 0)[0] for i in ids]
    mixing = fold_rows(pooled_all, jnp.concatenate(out_pieces, axis=0))
    residual = (local_rows.astype(jnp.float32) + mixing).astype(bf16)

    gathered_ffn = jnp.concatenate(tp_pieces(residual), axis=1)
    gate_mine = after(gate_mine, residual)
    gate_sent = others_of(gate_mine)
    gate_other = across_groups(gate_sent, gate_own)

    normed_ffn = norm_rows(gathered_ffn, pick_blocks(ffn_gain, ids))
    rows = gate_own[0].shape[0]
    ordered = []
    for which in whichs:
        for base in range(0, normed_ffn.shape[1], rows * parts):
            ordered.append(part_columns(normed_ffn[:, base : base + rows * parts], which, parts))
    operand = jnp.concatenate(ordered, axis=1)

    def wide(mine, others):
        blocks = row_blocks(mine, ids, lambda j: j)
        for other in others:
            blocks += row_blocks(other, ids, rel_place)
        return fold_rows(operand, jnp.concatenate(blocks, axis=0))

    up_mine = after(up_mine, operand)
    up_sent = others_of(up_mine)
    up_other = across_groups(up_sent, up_own)
    gate_other = [after(other, up_sent) for other in gate_other]
    gate_lin = (wide(gate_mine, gate_other) * gate_scale).astype(bf16)
    down_mine[0] = after(down_mine[0], gate_lin)
    down_sent = [others_of(down_mine[0])]
    down_other = [across_groups(down_sent[0], down_own[0])]
    up_other = [after(other, down_sent[0]) for other in up_other]
    up_lin = (wide(up_mine, up_other) * up_scale).astype(bf16)
    hidden = (jax.nn.silu(causal_taps(gate_lin, gate_taps)) * causal_taps(up_lin, up_taps)).astype(
        bf16
    )
    for chunk in range(1, chunks):
        down_mine[chunk] = after(down_mine[chunk], hidden)
        down_sent.append(others_of(down_mine[chunk]))
        down_other.append(across_groups(down_sent[chunk], down_own[chunk]))

    def same(j):
        return j

    stages = []
    for chunk in range(chunks):
        stages.append([(0, chunk, down_mine[chunk], same)])
        if chunk:
            stages[-1] += late
        late = [(1 + i, chunk, o, rel_place) for i, o in enumerate(down_other[chunk])]
    if late:
        stages.append(late)

    chips = tp_size // 2
    chip, core = tp_index // 2, tp_index % 2
    per_block = fs_size // tp_size
    found = {}
    for stage in stages:

        def product(block):
            weights = [column_block(stacked, block, place) for _, _, stacked, place in stage]
            return fold_rows(hidden, jnp.concatenate(weights, axis=1))

        total = None
        for step in list(range(1, chips)) + [0]:
            target = (chip + step) % chips
            other = tp_swap(product(target * 2 + 1 - core).astype(bf16))
            summed = product(target * 2 + core) + other.astype(jnp.float32)
            if step:
                summed = tp_step(summed.astype(bf16), step).astype(jnp.float32)
            total = summed if total is None else total + summed
        width = per_block * chunk_width
        for place, (part, chunk, _, _) in enumerate(stage):
            found[part, chunk] = total[:, place * width : (place + 1) * width]
    columns = []
    for j in range(per_block):
        for held in range(parts):
            for chunk in range(chunks):
                span = slice(j * chunk_width, (j + 1) * chunk_width)
                chosen = found[0, chunk][:, span]
                for step in range(1, parts):
                    chosen = jnp.where(whichs[step] == held, found[step, chunk][:, span], chosen)
                columns.append(chosen)
    feed_out = jnp.concatenate(columns, axis=1)
    result = (residual.astype(jnp.float32) + feed_out).astype(bf16)
    return result.reshape(1, length, result.shape[1])


def solution(mesh):
    return jax.shard_map(
        shards,
        mesh=mesh,
        in_specs=(
            P(("grp", "fs"), None, "tp"),
            P(),
            P("fs", "tp"),
            P(None, "tp"),
            P("tp", None, None),
            P(None, "tp"),
            P("tp", "fs"),
            P(None, "fs"),
            P(),
            P("fs", "tp"),
            P(None, "tp"),
            P("fs", "tp"),
            P(None, "tp"),
            P(None, "tp"),
            P(None, "tp"),
            P("tp", "fs"),
            P(None, "fs"),
        ),
        out_specs=P(("grp", "fs"), None, "tp"),
        check_vma=False,
    )
```

```python
import jax
import jax.numpy as jnp
from jax import lax
from jax.sharding import PartitionSpec as P


BLOCKS = 8


eps = 1e-06
widest_span = 16


def norm_rows(tok_rows, norm_gain):
    values = tok_rows.astype(jnp.float32)
    scaled = values * lax.rsqrt(jnp.mean(values * values, axis=-1, keepdims=True) + eps)
    return (scaled * norm_gain).astype(jnp.bfloat16)


def span_widths(block_ids):
    return jnp.left_shift(jnp.ones_like(block_ids), 1 + 4 * block_ids // BLOCKS)


def trailing_gap(projected, windows):
    values = projected.astype(jnp.float32)
    length = values.shape[0]
    running = values
    for offset in range(1, widest_span):
        shifted = jnp.pad(values[: length - offset], ((offset, 0), (0, 0)))
        running = running + jnp.where(windows[None, :] > offset, shifted, jnp.zeros_like(shifted))
    positions = jnp.arange(length, dtype=jnp.int32)[:, None]
    counts = jnp.minimum(positions + 1, windows[None, :]).astype(jnp.float32)
    return (running / counts - values).astype(jnp.bfloat16)


def causal_taps(linear, tap_table):
    values = linear.astype(jnp.float32)
    length = values.shape[0]
    back_one = jnp.pad(values[: length - 1], ((1, 0), (0, 0)))
    back_two = jnp.pad(values[: length - 2], ((2, 0), (0, 0)))
    return tap_table[2] * values + tap_table[1] * back_one + tap_table[0] * back_two


def fold_rows(operand, portion):
    return jnp.dot(operand, portion, preferred_element_type=jnp.float32)


def tp_swap(value):
    size = lax.axis_size("tp")
    return lax.ppermute(value, "tp", [(i, i ^ 1) for i in range(size)])


def tp_step(value, step):
    size = lax.axis_size("tp")
    chips = size // 2
    pairs = [(i, ((i // 2 + step) % chips) * 2 + i % 2) for i in range(size)]
    return lax.ppermute(value, "tp", pairs)


def tp_pieces(value):
    chips = lax.axis_size("tp") // 2
    near = [value] + [tp_step(value, step) for step in range(1, chips)]
    pieces = []
    for piece in near:
        pieces += [piece, tp_swap(piece)]
    return pieces


def tp_sources():
    chips = lax.axis_size("tp") // 2
    index = lax.axis_index("tp")
    ids = []
    for step in range(chips):
        chip = (index // 2 + chips - step) % chips
        ids += [chip * 2 + index % 2, chip * 2 + 1 - index % 2]
    return ids


def pick_blocks(array, ids, axis=0):
    width = array.shape[axis] // len(ids)
    return jnp.concatenate(
        [lax.dynamic_slice_in_dim(array, i * width, width, axis) for i in ids], axis
    )


def part_slice(array, which, parts, axis):
    width = array.shape[axis] // parts
    return lax.dynamic_slice_in_dim(array, which * width, width, axis)


def part_columns(array, which, parts):
    width = array.shape[1] // parts
    chosen = array[:, :width]
    for i in range(1, parts):
        chosen = jnp.where(which == i, array[:, i * width : (i + 1) * width], chosen)
    return chosen


def fs_stack(value):
    size = lax.axis_size("fs")
    index = lax.axis_index("fs")
    if size > 4:
        return lax.all_gather(value, "fs", axis=0, tiled=False), lambda j: j
    pieces = [value]
    for step in range(1, size):
        pairs = [(i, (i + step) % size) for i in range(size)]
        pieces.append(lax.ppermute(value, "fs", pairs))
    return jnp.stack(pieces), lambda j: (index - j + size) % size


def others_of(stacked):
    size = lax.axis_size("fs")
    index = lax.axis_index("fs")
    return jnp.concatenate(
        [lax.dynamic_slice_in_dim(stacked, (index + d) % size, 1, 0) for d in range(1, size)], 0
    )


def across_groups(sent, own_parts):
    parts = lax.axis_size("grp")
    found = []
    for step in range(1, parts):
        got = lax.ppermute(sent, "grp", [(i, (i - step) % parts) for i in range(parts)])
        found.append((own_parts[step], got))
    return found


def with_own(pairs, *earlier):
    return [jnp.concatenate([own[None], after(got, *earlier)], 0) for own, got in pairs]


def after(value, *earlier):
    return lax.optimization_barrier((value, *earlier))[0]


def rel_place(j):
    size = lax.axis_size("fs")
    return (j - lax.axis_index("fs") + size) % size


def row_blocks(stacked, ids, place):
    count = stacked.shape[0] // len(ids)
    return [
        lax.dynamic_slice_in_dim(stacked, place(i * count + j), 1, 0)[0]
        for i in ids
        for j in range(count)
    ]


def column_block(stacked, block, place):
    count = stacked.shape[0] // lax.axis_size("tp")
    return jnp.concatenate(row_blocks_of(stacked, block, count, place), axis=1)


def row_blocks_of(stacked, block, count, place):
    return [
        lax.dynamic_slice_in_dim(stacked, place(block * count + j), 1, 0)[0] for j in range(count)
    ]


def shards(
    tokens,
    mix_gain,
    in_matrix,
    in_scale,
    pool_mix,
    pool_scale,
    out_matrix,
    out_scale,
    ffn_gain,
    gate_matrix,
    gate_scale,
    up_matrix,
    up_scale,
    gate_taps,
    up_taps,
    down_matrix,
    down_scale,
):
    return layer(
        tokens,
        mix_gain,
        in_matrix,
        in_scale,
        pool_mix,
        pool_scale,
        out_matrix * out_scale,
        ffn_gain,
        gate_matrix,
        gate_scale,
        up_matrix,
        up_scale,
        gate_taps,
        up_taps,
        down_matrix * down_scale,
    )


def layer(
    tokens,
    mix_gain,
    in_matrix,
    in_scale,
    pool_mix,
    pool_scale,
    out_scaled,
    ffn_gain,
    gate_matrix,
    gate_scale,
    up_matrix,
    up_scale,
    gate_taps,
    up_taps,
    down_scaled,
):
    length = tokens.shape[1]
    own_width = tokens.shape[2]
    bf16 = jnp.bfloat16
    tp_index = lax.axis_index("tp")
    tp_size = lax.axis_size("tp")
    fs_size = lax.axis_size("fs")
    group = lax.axis_index("grp")
    parts = lax.axis_size("grp")
    ids = tp_sources()
    local_rows = tokens.reshape(length, own_width)
    gathered = jnp.concatenate(tp_pieces(local_rows), axis=1)
    in_stack, in_place = fs_stack(in_matrix.astype(bf16))
    out_stack, out_place = fs_stack(out_scaled.astype(bf16))

    whichs = [(group + step) % parts for step in range(parts)]
    gate_own = [part_slice(gate_matrix, which, parts, 0).astype(bf16) for which in whichs]
    up_own = [part_slice(up_matrix, which, parts, 0).astype(bf16) for which in whichs]
    half_width = down_scaled.shape[1] // parts
    chunks = 2 if half_width % 256 == 0 else 1
    chunk_width = half_width // chunks
    down_own = []
    for chunk in range(chunks):
        held = []
        for which in whichs:
            half = part_columns(down_scaled, which, parts).astype(bf16)
            held.append(half[:, chunk * chunk_width : (chunk + 1) * chunk_width])
        down_own.append(held)

    def gather(value):
        return lax.all_gather(value, "fs", axis=0, tiled=False)

    gate_mine = gather(gate_own[0])
    up_mine = gather(up_own[0])
    down_mine = [gather(down_own[c][0]) for c in range(chunks)]

    normed = norm_rows(gathered, pick_blocks(mix_gain, ids))
    width_in = in_matrix.shape[1]
    in_rows = jnp.concatenate(row_blocks(in_stack, ids, in_place), axis=0)
    projected = (fold_rows(normed, in_rows) * in_scale).astype(bf16)
    local_blocks = pool_mix.shape[0]
    block_width = pool_mix.shape[1]
    block_ids = tp_index * local_blocks + jnp.arange(local_blocks, dtype=jnp.int32)
    windows = jnp.repeat(span_widths(block_ids), block_width)
    spread = trailing_gap(projected, windows)
    block_mixed = jnp.einsum(
        "lbc,bce->lbe",
        spread.reshape(length, local_blocks, block_width),
        pool_mix,
        preferred_element_type=jnp.float32,
    ).reshape(length, width_in)
    pooled = (block_mixed * pool_scale).astype(bf16)
    out_blocks = jnp.stack([column_block(out_stack, i, out_place) for i in range(tp_size)])
    own_matrix = lax.all_to_all(out_blocks, "tp", split_axis=0, concat_axis=0, tiled=True)
    gate_mine = after(gate_mine, pooled)
    gate_sent = others_of(gate_mine)
    gate_other = across_groups(gate_sent, gate_own)
    own_matrix = after(own_matrix, gate_sent)
    pooled_all = jnp.concatenate(tp_pieces(pooled), axis=1)
    out_pieces = [lax.dynamic_slice_in_dim(own_matrix, i, 1, 0)[0] for i in ids]
    mixing = fold_rows(pooled_all, jnp.concatenate(out_pieces, axis=0))
    residual = (local_rows.astype(jnp.float32) + mixing).astype(bf16)

    gathered_ffn = jnp.concatenate(tp_pieces(residual), axis=1)
    normed_ffn = norm_rows(gathered_ffn, pick_blocks(ffn_gain, ids))
    rows = gate_own[0].shape[0]
    ordered = []
    for which in whichs:
        for base in range(0, normed_ffn.shape[1], rows * parts):
            ordered.append(part_columns(normed_ffn[:, base : base + rows * parts], which, parts))
    operand = jnp.concatenate(ordered, axis=1)

    def wide(mine, others):
        blocks = row_blocks(mine, ids, lambda j: j)
        for other in others:
            blocks += row_blocks(other, ids, rel_place)
        return fold_rows(operand, jnp.concatenate(blocks, axis=0))

    up_mine = after(up_mine, operand)
    up_sent = others_of(up_mine)
    up_other = across_groups(up_sent, up_own)
    gate_other = with_own(gate_other, up_sent)
    gate_lin = (wide(gate_mine, gate_other) * gate_scale).astype(bf16)
    down_mine[0] = after(down_mine[0], gate_lin)
    down_sent = [others_of(down_mine[0])]
    down_other = [across_groups(down_sent[0], down_own[0])]
    up_other = with_own(up_other, down_sent[0])
    up_lin = (wide(up_mine, up_other) * up_scale).astype(bf16)
    hidden = (jax.nn.silu(causal_taps(gate_lin, gate_taps)) * causal_taps(up_lin, up_taps)).astype(
        bf16
    )
    for chunk in range(1, chunks):
        down_mine[chunk] = after(down_mine[chunk], hidden)
        down_sent.append(others_of(down_mine[chunk]))
        down_other.append(across_groups(down_sent[chunk], down_own[chunk]))

    down_other = [with_own(pairs, hidden) for pairs in down_other]

    def same(j):
        return j

    stages = []
    for chunk in range(chunks):
        stages.append([(0, chunk, down_mine[chunk], same)])
        if chunk:
            stages[-1] += late
        late = [(1 + i, chunk, o, rel_place) for i, o in enumerate(down_other[chunk])]
    if late:
        stages.append(late)

    chips = tp_size // 2
    chip, core = tp_index // 2, tp_index % 2
    per_block = fs_size // tp_size
    found = {}
    for stage in stages:

        def product(block):
            weights = [column_block(stacked, block, place) for _, _, stacked, place in stage]
            return fold_rows(hidden, jnp.concatenate(weights, axis=1))

        total = None
        for step in list(range(1, chips)) + [0]:
            target = (chip + step) % chips
            other = tp_swap(product(target * 2 + 1 - core).astype(bf16))
            summed = product(target * 2 + core) + other.astype(jnp.float32)
            if step:
                summed = tp_step(summed.astype(bf16), step).astype(jnp.float32)
            total = summed if total is None else total + summed
        width = per_block * chunk_width
        for place, (part, chunk, _, _) in enumerate(stage):
            found[part, chunk] = total[:, place * width : (place + 1) * width]
    columns = []
    for j in range(per_block):
        for held in range(parts):
            for chunk in range(chunks):
                span = slice(j * chunk_width, (j + 1) * chunk_width)
                chosen = found[0, chunk][:, span]
                for step in range(1, parts):
                    chosen = jnp.where(whichs[step] == held, found[step, chunk][:, span], chosen)
                columns.append(chosen)
    feed_out = jnp.concatenate(columns, axis=1)
    result = (residual.astype(jnp.float32) + feed_out).astype(bf16)
    return result.reshape(1, length, result.shape[1])


def solution(mesh):
    return jax.shard_map(
        shards,
        mesh=mesh,
        in_specs=(
            P(("grp", "fs"), None, "tp"),
            P(),
            P("fs", "tp"),
            P(None, "tp"),
            P("tp", None, None),
            P(None, "tp"),
            P("tp", "fs"),
            P(None, "fs"),
            P(),
            P("fs", "tp"),
            P(None, "tp"),
            P("fs", "tp"),
            P(None, "tp"),
            P(None, "tp"),
            P(None, "tp"),
            P("tp", "fs"),
            P(None, "fs"),
        ),
        out_specs=P(("grp", "fs"), None, "tp"),
        check_vma=False,
    )
```
